32 devices in a mesh: grp: 2 (over y), ep: 4 (over z), tp: 4 (over x, core).
Axes of the slice: x: 2, y: 2, z: 4, core: 2. Of those that a mesh axis runs over, the one named last changes fastest.
Arguments:
- queries: bfloat16 [2048, 2048], P(('grp', 'ep'), 'tp'), parts along dimension 0, may hold values from -8 to 8
- keys: bfloat16 [2048, 512], P(('grp', 'ep')), parts along dimension 0, may hold values from -8 to 8
- values: bfloat16 [2048, 512], P(('grp', 'ep')), parts along dimension 0, may hold values from -6 to 6
- q_gain: float32 [128], replicated, may hold values from 0.6 to 5.8
- k_gain: float32 [128], replicated, may hold values from 0.6 to 5.8
- w_out: bfloat16 [2048, 2048], P(None, 'tp'), may hold values from -0.125 to 0.125
- moe_rows: bfloat16 [1536, 2048], P(('grp', 'ep')), parts along dimension 0, may hold values from -6 to 6
- routes: int32 [1536, 2], P(('grp', 'ep')), parts along dimension 0, may hold values from 0 to 3, all different within a row; in each aligned block of 192 rows (0 to 191, 192 to 383, ...) at most 144 rows name the same one
- group_gate: float32 [1536], P(('grp', 'ep')), parts along dimension 0, may hold values from 0.25 to 1
- expert_logits: float32 [1536, 2], P(('grp', 'ep')), parts along dimension 0, may hold values from -6 to 6
- moe_gain: float32 [2048], replicated, may hold values from 0.1 to 1.9
- w_gate: bfloat16 [4, 2048, 2048], P('ep', None, 'tp'), may hold values from -0.125 to 0.125
- w_up: bfloat16 [4, 2048, 2048], P('ep', None, 'tp'), may hold values from -0.125 to 0.125
- w_down: bfloat16 [4, 2048, 2048], P('ep', 'tp'), may hold values from -0.125 to 0.125
Outputs:
- attn_out: bfloat16 [2048, 2048], P(('grp', 'ep'), 'tp'), parts along dimension 0
- moe_out: bfloat16 [1536, 2048], P(('grp', 'ep'), 'tp'), parts along dimension 0
The draws below stay inside these ranges and needn't reach their ends.
There are 2 independent parts, one for each index of `grp`. The reference program is written for one: setup_inputs(seed, part) draws one part's arguments, and reference() takes and returns one part's arrays. A program takes and returns all parts, laid end to end along the dimension named above; an argument that names none is the same for every part. Nothing has to cross between parts.
Inputs may be any that keep to these rules, and one draw needn't show every extreme that they name: `routes`: each row names 2 different experts; within the rows of one index of ep no expert is named more than 144 times, a bound that some block reaches.
All inputs are finite; a program needn't handle non-finite values.
Results may differ from the reference program's by a relative error of at most 0.019.
The reference program's roundings to bfloat16 on the way count: a program that leaves them out, or rounds other values in their place, can miss the bound.
Values may be sent and summed in bfloat16 or wider, within the bound.
A program may use at most 64 MiB of HBM per device.

```python
import math
import jax
import jax.numpy as jnp
import numpy as np
from jax import lax

D = 2048
HEADS = 16
KV_HEADS = 4
HEAD_DIM = 128
GRID_W = 64
FF = 2048
TOPK = 2
MOE_DEV = 192
ATT_TOK = 1024
MOE_TOK = 768
EXPERTS = 4
CAP = 144
N_EP = 4
N_TP = 4


def drawn_keys(key):
    base = jax.random.normal(jax.random.fold_in(key, 7), (ATT_TOK, KV_HEADS * HEAD_DIM), jnp.float32)
    return jnp.clip(base, -8.0, 8.0)


def draw_keys(key, part):
    return drawn_keys(key).astype(jnp.bfloat16)


def draw_queries(key, part):
    own = jax.random.normal(jax.random.fold_in(key, 9), (ATT_TOK, HEADS * HEAD_DIM), jnp.float32)
    return jnp.clip(own, -8.0, 8.0).astype(jnp.bfloat16)


def draw_q_gain(key, part):
    return jax.random.uniform(jax.random.fold_in(key, 11), (HEAD_DIM,), jnp.float32, 0.6, 1.4)


def draw_k_gain(key, part):
    return jax.random.uniform(jax.random.fold_in(key, 13), (HEAD_DIM,), jnp.float32, 0.6, 1.4)


def block_levels(key, extent, cuts, least, high):
    level, own = 1.0, jax.random.fold_in(key, 6)
    for axis_at, shards_of in cuts:
        draws = jnp.exp(jax.random.uniform(jax.random.fold_in(own, axis_at), (shards_of,), jnp.float32, least / len(cuts), high / len(cuts)))
        level = level * jnp.repeat(draws, extent[axis_at] // shards_of).reshape([-1 if axis == axis_at else 1 for axis in range(len(extent))])
    return level


def shared_out(key, own, number, rows, number_of, top, most, skew):
    sequence = jax.random.permutation(key, number_of)
    heavy_load, usual = load_shares(number_of, rows * top, most, skew, True), load_shares(number_of, rows * top, most, skew, False)
    places = jnp.arange(number_of)

    def named(lengths, offset_by):
        used = int((lengths > 0).sum())
        fixed = max(1, used // 4)
        passed = fixed + (places - fixed + offset_by * (used - fixed)) % max(1, number_of - fixed)
        return jnp.zeros((number_of,), jnp.int32).at[sequence[jnp.where(places < fixed, places, passed)]].set(jnp.asarray(lengths, jnp.int32))

    lengths = jnp.where(number % 4 == 0, named(heavy_load, number // 4), named(usual, number - number // 4 - 1))
    mixed = jax.random.permutation(jax.random.fold_in(own, 3), number_of)
    giver, sink = mixed[0:number_of // 2 * 2:2], mixed[1:number_of // 2 * 2:2]
    slack = jnp.minimum(lengths[giver] - 1, most - lengths[sink]) // 2
    slack = jnp.where((giver == sequence[0]) | (sink == sequence[0]) | (lengths[sink] == 0), 0, jnp.maximum(slack, 0))
    passed = jax.random.randint(jax.random.fold_in(own, 4), (number_of // 2,), 0, 1 << 20) % (slack + 1)
    lengths = lengths.at[giver].add(-passed).at[sink].add(passed)
    members = jnp.searchsorted(jnp.cumsum(lengths), jnp.arange(rows * top), side="right").astype(jnp.int32)
    table = members.reshape(top, rows).T
    table = table[jax.random.permutation(jax.random.fold_in(own, 1), rows)]
    offset_by = jax.random.randint(jax.random.fold_in(own, 2), (rows, 1), 0, top)
    return jnp.take_along_axis(table, (jnp.arange(top)[None, :] + offset_by) % top, axis=1)


def load_shares(number_of, total, most, slope, full):
    weights = [(1 << 20) // math.isqrt(grade ** slope) + 1 for grade in range(1, number_of + 1)]
    largest = most if full else min(most, max(-(-total // number_of), total * weights[0] // sum(weights)))
    least = 1 if total - largest >= number_of - 1 else 0
    counts, rest = [largest] + [least] * (number_of - 1), total - largest - least * (number_of - 1)
    while rest > 0:
        free = [i for i in range(1, number_of) if counts[i] < largest] or [i for i in range(1, number_of) if counts[i] < most]
        mass, remaining = sum([weights[i] for i in free]), rest
        for i in free:
            addition = min(most - counts[i], max(1, remaining * weights[i] // mass), rest)
            counts[i] = counts[i] + addition
            rest = rest - addition
    return np.array(counts)


def bell_draw(rng, extent, deviation, reach, cuts=(), held_as=jnp.bfloat16):
    values = deviation * jax.random.normal(rng, extent, jnp.float32)
    if cuts:
        values = values * block_levels(rng, extent, cuts, -0.22, 0.18)
    return jnp.clip(values, -reach, reach).astype(held_as)


def setup_inputs(seed: int = 0, part: int = 0) -> dict:
    key_list = jax.random.split(jax.random.key(seed), 15)
    part_keys = jax.random.split(jax.random.fold_in(key_list[14], part), 15)
    queries = draw_queries(jax.random.fold_in(jax.random.fold_in(key_list[14], part), 71), part)
    keys = draw_keys(jax.random.fold_in(jax.random.fold_in(key_list[14], part), 71), part)
    values = bell_draw(part_keys[2], (ATT_TOK, KV_HEADS * HEAD_DIM), 1.0, 6.0, ((0, 4),))
    q_gain = draw_q_gain(jax.random.fold_in(key_list[14], 71), part)
    k_gain = draw_k_gain(jax.random.fold_in(key_list[14], 71), part)
    w_out = bell_draw(key_list[5], (HEADS * HEAD_DIM, D), (HEADS * HEAD_DIM) ** -0.5, 0.125, ((1, 4),))
    moe_rows = bell_draw(part_keys[6], (MOE_TOK, D), 1.0, 6.0, ((0, 4),))
    routes_keys = jax.random.split(jax.random.fold_in(part_keys[7], 1), MOE_TOK // MOE_DEV)
    routes_turns = jax.random.permutation(jax.random.fold_in(part_keys[7], 3), MOE_TOK // MOE_DEV)
    routes = jax.vmap(lambda own, number: shared_out(jax.random.fold_in(part_keys[7], 2), own, number, MOE_DEV, EXPERTS, TOPK, CAP, 1))(routes_keys, routes_turns).reshape((MOE_TOK, TOPK))
    group_gate = jnp.clip(jnp.exp(math.log(1.0) - 1.3862944 * jax.random.uniform(part_keys[8], (MOE_TOK,), jnp.float32) ** block_levels(part_keys[8], (MOE_TOK,), ((0, 4),), -0.2, 0.2)), 0.25, 1.0)
    expert_logits = bell_draw(part_keys[9], (MOE_TOK, TOPK), 1.5, 6.0, ((0, 4),), jnp.float32)
    moe_gain = jnp.clip(1.0 + 0.18 * jax.random.normal(key_list[10], (D,), jnp.float32), 0.1, 1.9)
    w_gate = bell_draw(key_list[11], (EXPERTS, D, FF), D ** -0.5, 0.125, ((0, 4), (2, 4)))
    w_up = bell_draw(key_list[12], (EXPERTS, D, FF), D ** -0.5, 0.125, ((0, 4), (2, 4)))
    w_down = bell_draw(key_list[13], (EXPERTS, FF, D), FF ** -0.5, 0.125, ((0, 4), (1, 4)))
    return {"queries": queries, "keys": keys, "values": values, "q_gain": q_gain, "k_gain": k_gain, "w_out": w_out, "moe_rows": moe_rows, "routes": routes, "group_gate": group_gate, "expert_logits": expert_logits, "moe_gain": moe_gain, "w_gate": w_gate, "w_up": w_up, "w_down": w_down}


def rope_tables(count):
    pos = jnp.arange(count, dtype=jnp.int32)
    row = (pos // GRID_W).astype(jnp.float32)
    col = (pos % GRID_W).astype(jnp.float32)
    nfreq = HEAD_DIM // 4
    inverse = 10000.0 ** (-jnp.arange(nfreq, dtype=jnp.float32) / nfreq)
    angle = jnp.concatenate([row[:, None] * inverse, row[:, None] * inverse, col[:, None] * inverse, col[:, None] * inverse], axis=1)
    return (jnp.cos(angle), jnp.sin(angle))

def rotate(x, cosine, sine):
    parts = x.reshape(x.shape[:-1] + (2, 2, HEAD_DIM // 4))
    turned = jnp.stack([-parts[..., 1, :], parts[..., 0, :]], axis=-2).reshape(x.shape)
    return x * cosine[:, None, :] + turned * sine[:, None, :]

def head_norm(x, gain):
    wide = x.astype(jnp.float32)
    return wide * lax.rsqrt(lax.optimization_barrier(jnp.mean(wide * wide, axis=-1, keepdims=True)) + 1e-06) * gain

def attend(query, key_rows, value_rows):
    scores = jnp.dot(query, key_rows.T, preferred_element_type=jnp.float32) * HEAD_DIM ** (-0.5)
    top = lax.optimization_barrier(jnp.max(scores, axis=-1, keepdims=True))
    expo = jnp.exp(scores - top)
    total = lax.optimization_barrier(jnp.sum(expo, axis=-1, keepdims=True))
    mixed = jnp.dot(expo.astype(jnp.bfloat16), value_rows, preferred_element_type=jnp.float32) / total
    return mixed.astype(jnp.bfloat16)

def slot_table(chosen):
    onehot = (chosen[:, None] == jnp.arange(EXPERTS, dtype=jnp.int32)[None, :]).astype(jnp.int32)
    rank = lax.optimization_barrier(jnp.sum((jnp.cumsum(onehot, axis=0) - onehot) * onehot, axis=1))
    return chosen * CAP + rank

def reference(queries, keys, values, q_gain, k_gain, w_out, moe_rows, routes, group_gate, expert_logits, moe_gain, w_gate, w_up, w_down):
    count = queries.shape[0]
    group = HEADS // KV_HEADS
    cosine, sine = rope_tables(count)
    q_rot = rotate(head_norm(queries.reshape(count, HEADS, HEAD_DIM), q_gain), cosine, sine).astype(jnp.bfloat16)
    k_rot = rotate(head_norm(keys.reshape(count, KV_HEADS, HEAD_DIM), k_gain), cosine, sine).astype(jnp.bfloat16)
    q_heads = q_rot.reshape(count, KV_HEADS, group, HEAD_DIM).transpose(1, 2, 0, 3)
    k_heads = k_rot.transpose(1, 0, 2)
    v_heads = values.reshape(count, KV_HEADS, HEAD_DIM).transpose(1, 0, 2)

    def per_key_head(items):
        q_group, key_rows, value_rows = items
        return lax.map(lambda query: attend(query, key_rows, value_rows), q_group)
    heads_out = lax.map(per_key_head, (q_heads, k_heads, v_heads))
    joined = heads_out.transpose(2, 0, 1, 3).reshape(count, HEADS * HEAD_DIM)
    attn_out = jnp.dot(joined, w_out, preferred_element_type=jnp.float32).astype(jnp.bfloat16)
    width = moe_rows.shape[1]
    wide = moe_rows.astype(jnp.float32)
    normed = (wide * lax.rsqrt(lax.optimization_barrier(jnp.mean(wide * wide, axis=-1, keepdims=True)) + 1e-06) * moe_gain).astype(jnp.bfloat16)
    blocks = normed.reshape(N_EP, MOE_DEV, width)
    chosen = routes.reshape(N_EP, MOE_DEV * TOPK)
    slots = jax.vmap(slot_table)(chosen)
    owner = jnp.arange(MOE_DEV * TOPK, dtype=jnp.int32) // TOPK

    def fill(block, slot):
        source = jnp.zeros((EXPERTS * CAP,), jnp.int32).at[slot].set(owner)
        used = jnp.zeros((EXPERTS * CAP,), jnp.bool_).at[slot].set(True)
        return jnp.where(used[:, None], block[source], jnp.zeros((), jnp.bfloat16))
    buffers = jax.vmap(fill)(blocks, slots)
    per_expert = buffers.reshape(N_EP, EXPERTS, CAP, width).transpose(1, 0, 2, 3).reshape(EXPERTS, N_EP * CAP, width)
    part_ff = FF // N_TP

    def expert(items):
        rows, gate_w, up_w, down_w = items
        gate = jnp.dot(rows, gate_w, preferred_element_type=jnp.float32)
        up = jnp.dot(rows, up_w, preferred_element_type=jnp.float32)
        hidden = (jax.nn.silu(gate) * up).astype(jnp.bfloat16)
        pieces = jnp.einsum('rtf,tfd->rtd', hidden.reshape(-1, N_TP, part_ff).astype(jnp.float32), down_w.reshape(N_TP, part_ff, width).astype(jnp.float32))
        return lax.optimization_barrier(jnp.sum(pieces.astype(jnp.bfloat16).astype(jnp.float32), axis=1)).astype(jnp.bfloat16)
    results = lax.map(expert, (per_expert, w_gate, w_up, w_down))
    by_source = results.reshape(EXPERTS, N_EP, CAP, width).transpose(1, 0, 2, 3).reshape(N_EP, EXPERTS * CAP, width)
    picked = jax.vmap(lambda table, slot: table[slot])(by_source, slots)
    picked = picked.astype(jnp.float32).reshape(N_EP * MOE_DEV, TOPK, width)
    weights = group_gate[:, None] * jax.nn.softmax(expert_logits, axis=-1)
    moe_out = lax.optimization_barrier(jnp.sum(weights[:, :, None] * picked, axis=1)).astype(jnp.bfloat16)
    return (attn_out, moe_out)
```

```python
import functools

import jax
import jax.numpy as jnp
import numpy as np
from jax import lax
from jax.experimental import pallas as pl
from jax.experimental.pallas import tpu as pltpu
from jax.sharding import PartitionSpec as P

HEADS = 16
KV_HEADS = 4
HEAD_DIM = 128
GRID_W = 64
TOPK = 2
CORES = 2
F32 = jnp.float32
BF16 = jnp.bfloat16
MESH = pl.DeviceIdType.MESH


def dot(a, b):
    return jnp.dot(a, b, preferred_element_type=F32)


def rope_tables(count):
    nfreq = HEAD_DIM // 4
    inverse = 10000.0 ** (-np.arange(nfreq, dtype=np.float32) / np.float32(nfreq))
    inverse = np.tile(inverse.astype(np.float32), 4)[None, :]
    sign = np.where(np.arange(HEAD_DIM) // nfreq % 2 == 0, -1.0, 1.0)[None, :]
    angle = np.arange(max(count, 8), dtype=np.float32)[:, None] * inverse
    wide = angle.astype(np.float64)
    return np.stack([np.cos(wide), np.sin(wide) * sign]).astype(np.float32)


def head_norm_rotate(x, gain, cosine, sine):
    wide = x.astype(F32)
    wide = wide * lax.rsqrt(jnp.mean(wide * wide, axis=-1, keepdims=True) + 1e-06) * gain
    n = HEAD_DIM // 4
    lane = lax.broadcasted_iota(jnp.int32, wide.shape, 1)
    turned = jnp.where(lane // n % 2 == 0, pltpu.roll(wide, HEAD_DIM - n, 1), pltpu.roll(wide, n, 1))
    return (wide * cosine + turned * sine).astype(BF16)


def kernel(
    E, T, C,
    q_ref, k_ref, v_ref, qg_ref, kg_ref, rowtab_ref, coltab_ref, rows_ref, routes_ref, routes_t_ref,
    gate_ref, logit_ref, mgain_ref, wo_hbm, wg_hbm, wu_hbm, wd_hbm,
    attn_ref, moe_ref,
    wo, wg, wu, wd, kvbuf, qrot, xn, dsend, xbuf, ysend, yown, yrecv, zsend, zrecv, fsend, back, obuf,
    cosb, sinb,
    w_sem, kv_s, kv_r, dp_s, dp_r, fw_s, fw_r, r1_s, r1_r, r2_s, r2_r, rt_s, rt_r, o_s, o_r, os_s, os_r,
):
    X = T // CORES
    ep, tp = lax.axis_index("ep"), lax.axis_index("tp")
    x, c = tp // CORES, tp % CORES
    sib = x * CORES + (1 - c)
    R, M, W = q_ref.shape[0], rows_ref.shape[0], rows_ref.shape[1]
    HW, F, HS, HO = W // 2, wg.shape[1], wd.shape[1] // T, q_ref.shape[1]
    heads_dev = HO // HEAD_DIM
    group = HEADS // KV_HEADS

    def peer_ep(d):
        return lax.rem(ep + (d + E) % E, E)

    def peer_x(d):
        return lax.rem(x + (d + X) % X, X) * CORES + c

    weights = [
        pltpu.make_async_copy(s, t, w_sem.at[i])
        for i, (s, t) in enumerate(((wg_hbm.at[0], wg), (wu_hbm.at[0], wu), (wd_hbm.at[0], wd), (wo_hbm, wo)))
    ]
    for w in weights:
        w.start()
    barrier = pltpu.get_barrier_semaphore()
    for d in range(1, E):
        pl.semaphore_signal(barrier, inc=1, device_id={"ep": peer_ep(d)}, device_id_type=MESH)
    for d in range(1, X):
        pl.semaphore_signal(barrier, inc=1, device_id={"tp": peer_x(d)}, device_id_type=MESH)
    pl.semaphore_signal(barrier, inc=1, device_id={"tp": sib}, device_id_type=MESH)

    sends = []

    def remote(src, dst, s, r, **where):
        return pltpu.make_async_remote_copy(
            src_ref=src, dst_ref=dst, send_sem=s, recv_sem=r, device_id=where, device_id_type=MESH
        )

    def send(*args, **where):
        copy = remote(*args, **where)
        copy.start()
        sends.append(copy)

    lane = lax.broadcasted_iota(jnp.int32, (GRID_W, HEAD_DIM), 1)
    for r in range(R // GRID_W):
        at = ep * (R // GRID_W) + r
        for i, buf in enumerate((cosb, sinb)):
            row = rowtab_ref[i, pl.ds(at, 1), :]
            buf[r * GRID_W : (r + 1) * GRID_W, :] = jnp.where(
                lane < HEAD_DIM // 2, jnp.broadcast_to(row, (GRID_W, HEAD_DIM)), coltab_ref[i, :GRID_W, :]
            )
    kv = pl.ds(pl.multiple_of(tp * heads_dev // group * HEAD_DIM, HEAD_DIM), HEAD_DIM)
    kvbuf[ep, 0] = head_norm_rotate(k_ref[:, kv], kg_ref[...], cosb[...], sinb[...])
    kvbuf[ep, 1] = v_ref[:, kv]

    wide = rows_ref[...].astype(F32)
    xn[...] = (
        wide * lax.rsqrt(jnp.mean(wide * wide, axis=-1, keepdims=True) + 1e-06) * mgain_ref[...]
    ).astype(BF16)

    def relative(v):
        return jnp.where(v >= ep, v - ep, v - ep + E)

    pad = -(-E // 16) * 16
    rt = relative(routes_t_ref[...])
    which = lax.broadcasted_iota(jnp.int32, (pad, M), 0)
    named = (which == rt[0:1, :]) | (which == rt[1:2, :])
    i0 = lax.broadcasted_iota(jnp.int32, (M, M), 0)
    i1 = lax.broadcasted_iota(jnp.int32, (M, M), 1)
    rank = dot(jnp.where(named, 1.0, 0.0).astype(BF16), jnp.where(i0 < i1, 1.0, 0.0).astype(BF16))
    rank = jnp.where(named, rank, -1.0)
    slot = lax.broadcasted_iota(jnp.int32, (C, M), 0).astype(F32)

    def picker(d):
        return jnp.where(slot == rank[d : d + 1, :], 1.0, 0.0).astype(BF16)

    pl.semaphore_wait(barrier, E - 1 + X - 1 + 1)
    for d in range(1, E):
        send(kvbuf.at[ep], kvbuf.at[ep], kv_s.at[d], kv_r.at[d], ep=peer_ep(d))
    half = pl.ds(pl.multiple_of(c * HW, 128), HW)
    for d in range(1, E):
        dsend[d] = dot(picker(d), xn[:, half]).astype(BF16)
        send(dsend.at[d], xbuf.at[d, c], dp_s.at[d], dp_r.at[d], ep=peer_ep(d))
    for h in range(2):
        xbuf[0, h] = dot(picker(0), xn[:, h * HW : (h + 1) * HW]).astype(BF16)

    for h in range(heads_dev):
        cols = slice(h * HEAD_DIM, (h + 1) * HEAD_DIM)
        qrot[:, cols] = head_norm_rotate(q_ref[:, cols], qg_ref[...], cosb[...], sinb[...])

    def arrive(d):
        remote(dsend.at[d], xbuf.at[d, c], dp_s.at[d], dp_r.at[d], ep=peer_ep(d)).wait_recv()
        send(xbuf.at[d, c], xbuf.at[d, c], fw_s.at[d], fw_r.at[d], tp=sib)

    def expert(d):
        if d:
            remote(xbuf.at[d, c], xbuf.at[d, 1 - c], fw_s.at[d], fw_r.at[d], tp=sib).wait_recv()
        x0, x1 = xbuf[d, 0], xbuf[d, 1]
        g = dot(x0, wg[:HW]) + dot(x1, wg[HW:])
        u = dot(x0, wu[:HW]) + dot(x1, wu[HW:])
        hidden = (g * jax.nn.sigmoid(g) * u).astype(BF16)
        for core, buf in ((1 - c, ysend), (c, yown)):
            for dx in range(X):
                t = lax.rem(x + dx, X) * CORES + core
                cols = pl.ds(pl.multiple_of(t * HS, HS), HS)
                buf[d, dx] = dot(hidden, wd[:, cols]).astype(BF16)
            if buf is ysend:
                send(ysend.at[d], yrecv.at[d], r1_s.at[d], r1_r.at[d], tp=sib)

    def pair(d):
        remote(ysend.at[d], yrecv.at[d], r1_s.at[d], r1_r.at[d], tp=sib).wait_recv()
        for dx in range(1, X):
            zsend[d, dx] = (yown[d, dx].astype(F32) + yrecv[d, dx].astype(F32)).astype(BF16)
            send(zsend.at[d, dx], zrecv.at[d, dx], r2_s.at[d, dx], r2_r.at[d, dx], tp=peer_x(dx))

    def total(d):
        value = yown[d, 0].astype(F32) + yrecv[d, 0].astype(F32)
        for dx in range(1, X):
            remote(
                zsend.at[d, dx], zrecv.at[d, dx], r2_s.at[d, dx], r2_r.at[d, dx], tp=peer_x(dx)
            ).wait_recv()
            value = value + zrecv[d, dx].astype(F32)
        if d == 0:
            back[0] = value.astype(BF16)
        else:
            fsend[d] = value.astype(BF16)
            send(fsend.at[d], back.at[d], rt_s.at[d], rt_r.at[d], ep=peer_ep(-d))

    for w in weights[:3]:
        w.wait()
    expert(0)

    for d in range(1, E):
        remote(kvbuf.at[ep], kvbuf.at[peer_ep(-d)], kv_s.at[d], kv_r.at[d], ep=peer_ep(d)).wait_recv()
    keys = kvbuf[:, 0].reshape(E * R, HEAD_DIM)
    vals = kvbuf[:, 1].reshape(E * R, HEAD_DIM)
    for h in range(heads_dev):
        cols = slice(h * HEAD_DIM, (h + 1) * HEAD_DIM)
        s = lax.dot_general(
            qrot[:, cols], keys, (((1,), (1,)), ((), ())), preferred_element_type=F32
        ) * HEAD_DIM ** (-0.5)
        e = jnp.exp(s - jnp.max(s, axis=-1, keepdims=True))
        l = jnp.sum(e, axis=-1, keepdims=True)
        obuf[tp, :, cols] = (dot(e.astype(BF16), vals) / l).astype(BF16)
    for dx in range(1, X):
        send(obuf.at[tp], obuf.at[tp], o_s.at[dx], o_r.at[dx], tp=peer_x(dx))
    send(obuf.at[tp], obuf.at[tp], os_s.at[0], os_r.at[0], tp=sib)

    def forward_heads():
        for dx in range(1, X):
            src = peer_x(-dx)
            remote(obuf.at[tp], obuf.at[src], o_s.at[dx], o_r.at[dx], tp=peer_x(dx)).wait_recv()
            send(obuf.at[src], obuf.at[src], os_s.at[dx], os_r.at[dx], tp=sib)

    def project():
        weights[3].wait()
        for dx in range(X):
            src = lax.rem(x + (X - dx) % X, X) * CORES + (1 - c)
            remote(obuf.at[tp], obuf.at[src], os_s.at[dx], os_r.at[dx], tp=sib).wait_recv()
        acc = dot(obuf[0], wo[:HO])
        for t in range(1, T):
            acc = acc + dot(obuf[t], wo[t * HO : (t + 1) * HO])
        attn_ref[...] = acc.astype(BF16)

    for d in range(1, E):
        arrive(d)
        pair(d - 1)
        expert(d)
        if d >= 2:
            total(d - 2)
    forward_heads()
    pair(E - 1)
    total(E - 2)
    project()
    total(E - 1)

    rm = relative(routes_ref[...])
    mwhich = lax.broadcasted_iota(jnp.int32, (M, 128), 1)
    first, second = mwhich == rm[:, 0:1], mwhich == rm[:, 1:2]
    mnamed = first | second
    mrank = dot(jnp.where(i1 < i0, 1.0, 0.0).astype(BF16), jnp.where(mnamed, 1.0, 0.0).astype(BF16))
    mrank = jnp.where(mnamed, mrank, -1.0)
    l0, l1 = logit_ref[:, 0:1], logit_ref[:, 1:2]
    top = jnp.maximum(l0, l1)
    e0, e1 = jnp.exp(l0 - top), jnp.exp(l1 - top)
    share0, share1 = gate_ref[...] * (e0 / (e0 + e1)), gate_ref[...] * (e1 / (e0 + e1))
    shares = jnp.where(first, share0, 0.0) + jnp.where(second, share1, 0.0)
    mslot = lax.broadcasted_iota(jnp.int32, (M, C), 1).astype(F32)
    out = jnp.zeros((M, HS), F32)
    for d in range(E):
        if d:
            remote(fsend.at[d], back.at[d], rt_s.at[d], rt_r.at[d], ep=peer_ep(-d)).wait_recv()
        pick = jnp.where(mslot == mrank[:, d : d + 1], 1.0, 0.0).astype(BF16)
        out = out + shares[:, d : d + 1] * dot(pick, back[d])
    moe_ref[...] = out.astype(BF16)
    for copy in sends:
        copy.wait_send()


def per_device(
    queries, keys, values, q_gain, k_gain, w_out, moe_rows, routes, group_gate, expert_logits, moe_gain,
    w_gate, w_up, w_down,
):
    E, T = lax.axis_size("ep"), lax.axis_size("tp")
    X = T // CORES
    R, HO = queries.shape
    M, W = moe_rows.shape
    F = w_gate.shape[2]
    HS = W // T
    C = -(-(3 * M // E) // 16) * 16
    vmem, hbm = pl.BlockSpec(memory_space=pltpu.VMEM), pl.BlockSpec(memory_space=pl.ANY)
    dma = lambda *shape: pltpu.SemaphoreType.DMA(shape)
    buf = lambda *shape: pltpu.VMEM(shape, BF16)
    return pl.pallas_call(
        functools.partial(kernel, E, T, C),
        out_shape=(jax.ShapeDtypeStruct((R, w_out.shape[1]), BF16), jax.ShapeDtypeStruct((M, HS), BF16)),
        in_specs=[vmem] * 13 + [hbm] * 4,
        out_specs=(vmem, vmem),
        scratch_shapes=[
            buf(*w_out.shape), buf(W, F), buf(W, F), buf(F, W),
            buf(E, 2, R, HEAD_DIM), buf(R, HO), buf(M, W), buf(E, C, W // 2), buf(E, 2, C, W // 2),
            buf(E, X, C, HS), buf(E, X, C, HS), buf(E, X, C, HS), buf(E, X, C, HS), buf(E, X, C, HS),
            buf(E, C, HS), buf(E, C, HS), buf(T, R, HO),
            pltpu.VMEM((R, HEAD_DIM), F32), pltpu.VMEM((R, HEAD_DIM), F32),
            dma(4), dma(E), dma(E), dma(E), dma(E), dma(E), dma(E), dma(E), dma(E),
            dma(E, X), dma(E, X), dma(E), dma(E), dma(X), dma(X), dma(X), dma(X),
        ],
        compiler_params=pltpu.CompilerParams(
            collective_id=0, has_side_effects=True, vmem_limit_bytes=56 * 1024 * 1024
        ),
        name="layer",
    )(
        queries, keys, values, q_gain[None], k_gain[None],
        jnp.asarray(rope_tables(R * E // GRID_W)), jnp.asarray(rope_tables(GRID_W)),
        moe_rows, routes, routes.T, group_gate[:, None], expert_logits, moe_gain[None],
        w_out, w_gate, w_up, w_down,
    )


def solution(mesh):
    placed = (
        P(("grp", "ep"), "tp"),
        P(("grp", "ep"), None),
        P(("grp", "ep"), None),
        P(),
        P(),
        P(None, "tp"),
        P(("grp", "ep"), None),
        P(("grp", "ep"), None),
        P(("grp", "ep")),
        P(("grp", "ep"), None),
        P(),
        P("ep", None, "tp"),
        P("ep", None, "tp"),
        P("ep", "tp", None),
    )
    return jax.shard_map(
        per_device,
        mesh=mesh,
        in_specs=placed,
        out_specs=(P(("grp", "ep"), "tp"), P(("grp", "ep"), "tp")),
        check_vma=False,
    )
```

```python
import functools

import jax
import jax.numpy as jnp
import numpy as np
from jax import lax
from jax.experimental import pallas as pl
from jax.experimental.pallas import tpu as pltpu
from jax.sharding import PartitionSpec as P

HEADS = 16
KV_HEADS = 4
HEAD_DIM = 128
GRID_W = 64
TOPK = 2
CORES = 2
F32 = jnp.float32
BF16 = jnp.bfloat16
MESH = pl.DeviceIdType.MESH


def dot(a, b):
    return jnp.dot(a, b, preferred_element_type=F32)


def rope_tables(count):
    nfreq = HEAD_DIM // 4
    inverse = 10000.0 ** (-np.arange(nfreq, dtype=np.float32) / np.float32(nfreq))
    inverse = np.tile(inverse.astype(np.float32), 4)[None, :]
    sign = np.where(np.arange(HEAD_DIM) // nfreq % 2 == 0, -1.0, 1.0)[None, :]
    angle = np.arange(max(count, 8), dtype=np.float32)[:, None] * inverse
    wide = angle.astype(np.float64)
    return np.stack([np.cos(wide), np.sin(wide) * sign]).astype(np.float32)


def head_norm_rotate(x, gain, cosine, sine):
    wide = x.astype(F32)
    wide = wide * lax.rsqrt(jnp.mean(wide * wide, axis=-1, keepdims=True) + 1e-06) * gain
    n = HEAD_DIM // 4
    lane = lax.broadcasted_iota(jnp.int32, wide.shape, 1)
    turned = jnp.where(lane // n % 2 == 0, pltpu.roll(wide, HEAD_DIM - n, 1), pltpu.roll(wide, n, 1))
    return (wide * cosine + turned * sine).astype(BF16)


def kernel(
    E, T, C,
    q_ref, k_ref, v_ref, qg_ref, kg_ref, rowtab_ref, coltab_ref, rows_ref, routes_ref,
    gate_ref, logit_ref, mgain_ref, wo_hbm, wg_hbm, wu_hbm, wd_hbm,
    attn_ref, moe_ref,
    wo, wg, wu, wd, kvbuf, qrot, xn, dsend, xbuf, ysend, yown, yrecv, zsend, zrecv, fsend, back, obuf,
    cosb, sinb,
    w_sem, kv_s, kv_r, dp_s, dp_r, dx_s, dx_r, fw_s, fw_r, r1_s, r1_r, r2_s, r2_r, rt_s, rt_r, o_s, o_r, os_s, os_r,
):
    X = T // CORES
    ep, tp = lax.axis_index("ep"), lax.axis_index("tp")
    x, c = tp // CORES, tp % CORES
    sib = x * CORES + (1 - c)
    R, M, W = q_ref.shape[0], rows_ref.shape[0], rows_ref.shape[1]
    F, HS, HO = wg.shape[1], wd.shape[1] // T, q_ref.shape[1]
    heads_dev = HO // HEAD_DIM
    group = HEADS // KV_HEADS

    def peer_ep(d):
        return lax.rem(ep + (d + E) % E, E)

    def peer_x(d):
        return lax.rem(x + (d + X) % X, X) * CORES + c

    weights = [
        pltpu.make_async_copy(s, t, w_sem.at[i])
        for i, (s, t) in enumerate(((wg_hbm.at[0], wg), (wu_hbm.at[0], wu), (wd_hbm.at[0], wd), (wo_hbm, wo)))
    ]
    for w in weights:
        w.start()
    barrier = pltpu.get_barrier_semaphore()
    for d in range(1, E):
        pl.semaphore_signal(barrier, inc=1, device_id={"ep": peer_ep(d)}, device_id_type=MESH)
    for d in range(1, X):
        pl.semaphore_signal(barrier, inc=1, device_id={"tp": peer_x(d)}, device_id_type=MESH)
    pl.semaphore_signal(barrier, inc=1, device_id={"tp": sib}, device_id_type=MESH)

    sends = []

    def remote(src, dst, s, r, **where):
        return pltpu.make_async_remote_copy(
            src_ref=src, dst_ref=dst, send_sem=s, recv_sem=r, device_id=where, device_id_type=MESH
        )

    def send(*args, **where):
        copy = remote(*args, **where)
        copy.start()
        sends.append(copy)

    wide = rows_ref[...].astype(F32)
    xn[...] = (
        wide * lax.rsqrt(jnp.mean(wide * wide, axis=-1, keepdims=True) + 1e-06) * mgain_ref[...]
    ).astype(BF16)

    def relative(v):
        return jnp.where(v >= ep, v - ep, v - ep + E)

    pad = -(-E // 16) * 16
    rt = relative(routes_ref[...])
    which = lax.broadcasted_iota(jnp.int32, (pad, M), 0)
    first, second = which == rt[0:1, :], which == rt[1:2, :]
    named = first | second
    i0 = lax.broadcasted_iota(jnp.int32, (M, M), 0)
    i1 = lax.broadcasted_iota(jnp.int32, (M, M), 1)
    rank = dot(jnp.where(named, 1.0, 0.0).astype(BF16), jnp.where(i0 < i1, 1.0, 0.0).astype(BF16))
    rank = jnp.where(named, rank, -1.0)
    slot = lax.broadcasted_iota(jnp.int32, (C, M), 0).astype(F32)

    def picker(d):
        return jnp.where(slot == rank[d : d + 1, :], 1.0, 0.0).astype(BF16)

    mine = pl.ds(pl.multiple_of(tp * HS, 128), HS)
    for d in range(1, E):
        dsend[d] = dot(picker(d), xn[:, mine]).astype(BF16)
        if d == 1:
            pl.semaphore_wait(barrier, E - 1 + X - 1 + 1)
        send(dsend.at[d], xbuf.at[d, tp], dp_s.at[d], dp_r.at[d], ep=peer_ep(d))

    lane = lax.broadcasted_iota(jnp.int32, (GRID_W, HEAD_DIM), 1)
    for r in range(R // GRID_W):
        at = ep * (R // GRID_W) + r
        for i, buf in enumerate((cosb, sinb)):
            row = rowtab_ref[i, pl.ds(at, 1), :]
            buf[r * GRID_W : (r + 1) * GRID_W, :] = jnp.where(
                lane < HEAD_DIM // 2, jnp.broadcast_to(row, (GRID_W, HEAD_DIM)), coltab_ref[i, :GRID_W, :]
            )
    kv = pl.ds(pl.multiple_of(tp * heads_dev // group * HEAD_DIM, HEAD_DIM), HEAD_DIM)
    kvbuf[ep, 0] = head_norm_rotate(k_ref[:, kv], kg_ref[...], cosb[...], sinb[...])
    kvbuf[ep, 1] = v_ref[:, kv]

    for d in range(1, E):
        send(kvbuf.at[ep], kvbuf.at[ep], kv_s.at[d], kv_r.at[d], ep=peer_ep(d))
    for t in range(T):
        xbuf[0, t] = dot(picker(0), xn[:, t * HS : (t + 1) * HS]).astype(BF16)

    for h in range(heads_dev):
        cols = slice(h * HEAD_DIM, (h + 1) * HEAD_DIM)
        qrot[:, cols] = head_norm_rotate(q_ref[:, cols], qg_ref[...], cosb[...], sinb[...])

    def arrive(d):
        own = xbuf.at[d, tp]
        remote(dsend.at[d], own, dp_s.at[d], dp_r.at[d], ep=peer_ep(d)).wait_recv()
        for dx in range(1, X):
            send(own, own, dx_s.at[d, dx], dx_r.at[d, dx], tp=peer_x(dx))
        send(own, own, fw_s.at[d, 0], fw_r.at[d, 0], tp=sib)

    def relay(d):
        for dx in range(1, X):
            theirs = xbuf.at[d, peer_x(-dx)]
            remote(xbuf.at[d, tp], theirs, dx_s.at[d, dx], dx_r.at[d, dx], tp=peer_x(dx)).wait_recv()
            send(theirs, theirs, fw_s.at[d, dx], fw_r.at[d, dx], tp=sib)

    def expert(d):
        if d:
            for dx in range(X):
                theirs = xbuf.at[d, lax.rem(x + (X - dx) % X, X) * CORES + (1 - c)]
                remote(xbuf.at[d, tp], theirs, fw_s.at[d, dx], fw_r.at[d, dx], tp=sib).wait_recv()
        rows = jnp.concatenate([xbuf[d, t] for t in range(T)], axis=1)
        g, u = dot(rows, wg[...]), dot(rows, wu[...])
        hidden = (g * jax.nn.sigmoid(g) * u).astype(BF16)
        for core, buf in ((1 - c, ysend), (c, yown)):
            for dx in range(X):
                t = lax.rem(x + dx, X) * CORES + core
                cols = pl.ds(pl.multiple_of(t * HS, HS), HS)
                buf[d, dx] = dot(hidden, wd[:, cols]).astype(BF16)
            if buf is ysend:
                send(ysend.at[d], yrecv.at[d], r1_s.at[d], r1_r.at[d], tp=sib)

    def pair(d):
        remote(ysend.at[d], yrecv.at[d], r1_s.at[d], r1_r.at[d], tp=sib).wait_recv()
        for dx in range(1, X):
            zsend[d, dx] = (yown[d, dx].astype(F32) + yrecv[d, dx].astype(F32)).astype(BF16)
            send(zsend.at[d, dx], zrecv.at[d, dx], r2_s.at[d, dx], r2_r.at[d, dx], tp=peer_x(dx))

    def total(d):
        value = yown[d, 0].astype(F32) + yrecv[d, 0].astype(F32)
        for dx in range(1, X):
            remote(
                zsend.at[d, dx], zrecv.at[d, dx], r2_s.at[d, dx], r2_r.at[d, dx], tp=peer_x(dx)
            ).wait_recv()
            value = value + zrecv[d, dx].astype(F32)
        if d == 0:
            back[0] = value.astype(BF16)
        else:
            fsend[d] = value.astype(BF16)
            send(fsend.at[d], back.at[d], rt_s.at[d], rt_r.at[d], ep=peer_ep(-d))

    def forward_heads():
        for dx in range(1, X):
            src = peer_x(-dx)
            remote(obuf.at[tp], obuf.at[src], o_s.at[dx], o_r.at[dx], tp=peer_x(dx)).wait_recv()
            send(obuf.at[src], obuf.at[src], os_s.at[dx], os_r.at[dx], tp=sib)

    def project():
        weights[3].wait()
        for dx in range(X):
            src = lax.rem(x + (X - dx) % X, X) * CORES + (1 - c)
            remote(obuf.at[tp], obuf.at[src], os_s.at[dx], os_r.at[dx], tp=sib).wait_recv()
        acc = dot(obuf[0], wo[:HO])
        for t in range(1, T):
            acc = acc + dot(obuf[t], wo[t * HO : (t + 1) * HO])
        attn_ref[...] = acc.astype(BF16)

    def attend():
        for d in range(1, E):
            remote(kvbuf.at[ep], kvbuf.at[peer_ep(-d)], kv_s.at[d], kv_r.at[d], ep=peer_ep(d)).wait_recv()
        keys = kvbuf[:, 0].reshape(E * R, HEAD_DIM)
        vals = kvbuf[:, 1].reshape(E * R, HEAD_DIM)
        for h in range(heads_dev):
            cols = slice(h * HEAD_DIM, (h + 1) * HEAD_DIM)
            s = lax.dot_general(
                qrot[:, cols], keys, (((1,), (1,)), ((), ())), preferred_element_type=F32
            ) * HEAD_DIM ** (-0.5)
            e = jnp.exp(s - jnp.max(s, axis=-1, keepdims=True))
            l = jnp.sum(e, axis=-1, keepdims=True)
            obuf[tp, :, cols] = (dot(e.astype(BF16), vals) / l).astype(BF16)
        for dx in range(1, X):
            send(obuf.at[tp], obuf.at[tp], o_s.at[dx], o_r.at[dx], tp=peer_x(dx))
        send(obuf.at[tp], obuf.at[tp], os_s.at[0], os_r.at[0], tp=sib)

    for w in weights[:3]:
        w.wait()
    expert(0)
    arrive(1)
    pair(0)
    for d in range(1, E):
        relay(d)
        if d + 1 < E:
            arrive(d + 1)
        expert(d)
        total(d - 1)
        pair(d)
    attend()
    total(E - 1)
    forward_heads()
    project()

    l0, l1 = logit_ref[0:1, :], logit_ref[1:2, :]
    top = jnp.maximum(l0, l1)
    e0, e1 = jnp.exp(l0 - top), jnp.exp(l1 - top)
    share0, share1 = gate_ref[...] * (e0 / (e0 + e1)), gate_ref[...] * (e1 / (e0 + e1))
    shares = (jnp.where(first, share0, 0.0) + jnp.where(second, share1, 0.0)).T
    mrank = rank.T
    mslot = lax.broadcasted_iota(jnp.int32, (M, C), 1).astype(F32)
    out = jnp.zeros((M, HS), F32)
    for d in range(E):
        if d:
            remote(fsend.at[d], back.at[d], rt_s.at[d], rt_r.at[d], ep=peer_ep(-d)).wait_recv()
        pick = jnp.where(mslot == mrank[:, d : d + 1], 1.0, 0.0).astype(BF16)
        out = out + shares[:, d : d + 1] * dot(pick, back[d])
    moe_ref[...] = out.astype(BF16)
    for copy in sends:
        copy.wait_send()


def hand_over(a_ref, b_ref, attn_ref, moe_ref):
    attn_ref[...] = a_ref[...]
    moe_ref[...] = b_ref[...]


def per_device(
    queries, keys, values, q_gain, k_gain, w_out, moe_rows, routes, group_gate, expert_logits, moe_gain,
    w_gate, w_up, w_down,
):
    E, T = lax.axis_size("ep"), lax.axis_size("tp")
    X = T // CORES
    R, HO = queries.shape
    M, W = moe_rows.shape
    F = w_gate.shape[2]
    HS = W // T
    C = -(-(3 * M // E) // 16) * 16
    vmem, hbm = pl.BlockSpec(memory_space=pltpu.VMEM), pl.BlockSpec(memory_space=pl.ANY)
    dma = lambda *shape: pltpu.SemaphoreType.DMA(shape)
    buf = lambda *shape: pltpu.VMEM(shape, BF16)
    outs = pl.pallas_call(
        functools.partial(kernel, E, T, C),
        out_shape=(jax.ShapeDtypeStruct((R, w_out.shape[1]), BF16), jax.ShapeDtypeStruct((M, HS), BF16)),
        in_specs=[vmem] * 12 + [hbm] * 4,
        out_specs=(vmem, vmem),
        scratch_shapes=[
            buf(*w_out.shape), buf(W, F), buf(W, F), buf(F, W),
            buf(E, 2, R, HEAD_DIM), buf(R, HO), buf(M, W), buf(E, C, HS), buf(E, T, C, HS),
            buf(E, X, C, HS), buf(E, X, C, HS), buf(E, X, C, HS), buf(E, X, C, HS), buf(E, X, C, HS),
            buf(E, C, HS), buf(E, C, HS), buf(T, R, HO),
            pltpu.VMEM((R, HEAD_DIM), F32), pltpu.VMEM((R, HEAD_DIM), F32),
            dma(4), dma(E), dma(E), dma(E), dma(E), dma(E, X), dma(E, X), dma(E, X), dma(E, X), dma(E), dma(E),
            dma(E, X), dma(E, X), dma(E), dma(E), dma(X), dma(X), dma(X), dma(X),
        ],
        compiler_params=pltpu.CompilerParams(
            collective_id=0, has_side_effects=True, vmem_limit_bytes=56 * 1024 * 1024
        ),
        name="layer",
    )(
        queries, keys, values, q_gain[None], k_gain[None],
        jnp.asarray(rope_tables(R * E // GRID_W)), jnp.asarray(rope_tables(GRID_W)),
        moe_rows, routes.T, group_gate[None], expert_logits.T, moe_gain[None],
        w_out, w_gate, w_up, w_down,
    )
    return pl.pallas_call(
        hand_over, out_shape=tuple(jax.ShapeDtypeStruct(o.shape, BF16) for o in outs),
        in_specs=[vmem] * 2, out_specs=(vmem, vmem), name="hand_over",
    )(*outs)


def solution(mesh):
    placed = (
        P(("grp", "ep"), "tp"),
        P(("grp", "ep"), None),
        P(("grp", "ep"), None),
        P(),
        P(),
        P(None, "tp"),
        P(("grp", "ep"), None),
        P(("grp", "ep"), None),
        P(("grp", "ep")),
        P(("grp", "ep"), None),
        P(),
        P("ep", None, "tp"),
        P("ep", None, "tp"),
        P("ep", "tp", None),
    )
    return jax.shard_map(
        per_device,
        mesh=mesh,
        in_specs=placed,
        out_specs=(P(("grp", "ep"), "tp"), P(("grp", "ep"), "tp")),
        check_vma=False,
    )
```
